32 devices in a mesh: ep: 8 (over z, y), tp: 4 (over x, core).
Axes of the slice: x: 2, y: 2, z: 4, core: 2. Of those that a mesh axis runs over, the one named last changes fastest.
Arguments:
- tokens: bfloat16 [24, 2048], P('ep'), may hold values from -6 to 6
- pre_gain: float32 [2048], replicated, may hold values from 0.1 to 1.9
- w_query: bfloat16 [2048, 2048], P('tp', 'ep'), may hold values from -0.125 to 0.125
- w_forget: bfloat16 [2048, 2048], P('tp', 'ep'), may hold values from -0.125 to 0.125
- w_input: bfloat16 [2048, 2048], P('tp', 'ep'), may hold values from -0.125 to 0.125
- w_outgate: bfloat16 [2048, 2048], P('tp', 'ep'), may hold values from -0.125 to 0.125
- lower_bound: float32 [2048], P('tp'), may hold values from 0 to 0.9
- head_gain: float32 [2048], P('tp'), may hold values from 0.1 to 1.9
- w_output: bfloat16 [2048, 2048], P('tp', 'ep'), may hold values from -0.125 to 0.125
- mix_gain: float32 [2048], replicated, may hold values from 0.1 to 1.9
- ffn_gain: float32 [2048], replicated, may hold values from 0.1 to 1.9
- post_gain: float32 [2048], replicated, may hold values from 0.1 to 1.9
- state: float32 [24, 16, 128, 128], P('ep', 'tp'), may hold values from -4 to 4
- routes: int32 [24, 2], P('ep'), may hold values from 0 to 7, all different within a row; in each aligned block of 24 rows (0 to 23, 24 to 47, ...) at most 12 rows name the same one
- route_scores: float32 [24, 2], P('ep'), may hold values from 0.1 to 1
- w_gate: bfloat16 [8, 2048, 512], P('ep', None, 'tp'), may hold values from -0.125 to 0.125
- w_up: bfloat16 [8, 2048, 512], P('ep', None, 'tp'), may hold values from -0.125 to 0.125
- w_down: bfloat16 [8, 512, 2048], P('ep', 'tp'), may hold values from -0.25 to 0.25
Outputs:
- layer_out: bfloat16 [24, 2048], P('ep')
- new_state: float32 [24, 16, 128, 128], P('ep', 'tp')
The draws below stay inside these ranges and needn't reach their ends.
Inputs may be any that keep to these rules, and one draw needn't show every extreme that they name: `routes`: over all 24 tokens no expert is named more than 12 times, a bound that some block reaches; a row never names one expert twice.
All inputs are finite; a program needn't handle non-finite values.
Results may differ from the reference program's by a relative error of at most 0.023.
Values may be sent and summed in bfloat16 or wider, within the bound.
A program may use at most 64 MiB of HBM per device.

```python
import math
import jax
import jax.numpy as jnp
import numpy as np
from jax import lax

D = 2048
HEAD = 128
HEADS = 16
FF = 512
EXPERTS = 8
TOPK = 2
SEQS = 24
CAP = 12
N_TP = 4


def level_of(rng, shape, shards, smallest, high):
    def one(dim, parts):
        steps = jax.random.uniform(jax.random.fold_in(jax.random.fold_in(rng, 6), dim), (parts,), jnp.float32, smallest / len(shards), high / len(shards))
        return jnp.repeat(jnp.exp(steps), shape[dim] // parts).reshape((-1,) + (1,) * (len(shape) - dim - 1))

    factor_of = one(*shards[0])
    for cut in shards[1:]:
        factor_of = factor_of * one(*cut)
    return factor_of


def deal_out(stream_key, own, number, rows, amount, top, reach, lean):
    order = jax.random.permutation(stream_key, amount)
    heavy_load, common = load_shares(amount, rows * top, reach, lean, True), load_shares(amount, rows * top, reach, lean, False)
    places = jnp.arange(amount)

    def named(lengths, rotation):
        used = int((lengths > 0).sum())
        fixed = max(1, used // 4)
        passed = fixed + (places - fixed + rotation * (used - fixed)) % max(1, amount - fixed)
        return jnp.zeros((amount,), jnp.int32).at[order[jnp.where(places < fixed, places, passed)]].set(jnp.asarray(lengths, jnp.int32))

    lengths = jnp.where(number % 4 == 0, named(heavy_load, number // 4), named(common, number - number // 4 - 1))
    mixed = jax.random.permutation(jax.random.fold_in(own, 3), amount)
    giver, taker = mixed[0:amount // 2 * 2:2], mixed[1:amount // 2 * 2:2]
    margin = jnp.minimum(lengths[giver] - 1, reach - lengths[taker]) // 2
    margin = jnp.where((giver == order[0]) | (taker == order[0]) | (lengths[taker] == 0), 0, jnp.maximum(margin, 0))
    passed = jax.random.randint(jax.random.fold_in(own, 4), (amount // 2,), 0, 1 << 20) % (margin + 1)
    lengths = lengths.at[giver].add(-passed).at[taker].add(passed)
    items = jnp.searchsorted(jnp.cumsum(lengths), jnp.arange(rows * top), side="right").astype(jnp.int32)
    table = items.reshape(top, rows).T
    table = table[jax.random.permutation(jax.random.fold_in(own, 1), rows)]
    rotation = jax.random.randint(jax.random.fold_in(own, 2), (rows, 1), 0, top)
    return jnp.take_along_axis(table, (jnp.arange(top)[None, :] + rotation) % top, axis=1)


def load_shares(number_of, total, reach, slope, full):
    loads = [(1 << 20) // math.isqrt(grade ** slope) + 1 for grade in range(1, number_of + 1)]
    largest = reach if full else min(reach, max(-(-total // number_of), total * loads[0] // sum(loads)))
    least = 1 if total - largest >= number_of - 1 else 0
    given, surplus = [largest] + [least] * (number_of - 1), total - largest - least * (number_of - 1)
    while surplus > 0:
        free = [i for i in range(1, number_of) if given[i] < largest] or [i for i in range(1, number_of) if given[i] < reach]
        mass, budget = sum([loads[i] for i in free]), surplus
        for i in free:
            extra = min(reach - given[i], max(1, budget * loads[i] // mass), surplus)
            given[i] = given[i] + extra
            surplus = surplus - extra
    return np.array(given)


def bell_draw(key, extent, scale, reach, pieces=(), kind=jnp.bfloat16):
    array = jax.random.normal(key, extent, jnp.float32) * scale
    if len(pieces) > 0:
        array = level_of(key, extent, pieces, -0.22, 0.18) * array
    return jnp.clip(array, min=-reach, max=reach).astype(kind)


def setup_inputs(seed: int = 0) -> dict:
    seeds = jax.random.split(jax.random.key(seed), 19)
    tokens = bell_draw(seeds[0], (SEQS, D), 1.0, 6.0, ((0, 8),))
    pre_gain = jnp.clip(1.0 + 0.18 * jax.random.normal(seeds[1], (D,), jnp.float32), 0.1, 1.9)
    w_query = bell_draw(seeds[2], (D, D), D ** -0.5, 0.125, ((0, 4), (1, 8)))
    w_forget = bell_draw(seeds[3], (D, D), D ** -0.5, 0.125, ((0, 4), (1, 8)))
    w_input = bell_draw(seeds[4], (D, D), D ** -0.5, 0.125, ((0, 4), (1, 8)))
    w_outgate = bell_draw(seeds[5], (D, D), D ** -0.5, 0.125, ((0, 4), (1, 8)))
    lower_bound = jnp.clip(0.9 * jax.random.uniform(seeds[6], (D,), jnp.float32) ** level_of(seeds[6], (D,), ((0, 4),), -0.2, 0.2), 0.0, 0.9)
    head_gain = jnp.clip(1.0 + 0.18 * jax.random.normal(seeds[7], (D,), jnp.float32), 0.1, 1.9)
    w_output = bell_draw(seeds[8], (D, D), D ** -0.5, 0.125, ((0, 4), (1, 8)))
    mix_gain = jnp.clip(1.0 + 0.18 * jax.random.normal(seeds[9], (D,), jnp.float32), 0.1, 1.9)
    ffn_gain = jnp.clip(1.0 + 0.18 * jax.random.normal(seeds[10], (D,), jnp.float32), 0.1, 1.9)
    post_gain = jnp.clip(1.0 + 0.18 * jax.random.normal(seeds[11], (D,), jnp.float32), 0.1, 1.9)
    state = bell_draw(seeds[12], (SEQS, HEADS, HEAD, HEAD), 0.5, 4.0, ((0, 8), (1, 4)), jnp.float32)
    routes_keys = jax.random.split(jax.random.fold_in(seeds[13], 1), SEQS // SEQS)
    routes_turns = jax.random.permutation(jax.random.fold_in(seeds[13], 3), SEQS // SEQS)
    routes = jax.vmap(lambda own, number: deal_out(jax.random.fold_in(seeds[13], 2), own, number, SEQS, EXPERTS, TOPK, CAP, 2))(routes_keys, routes_turns).reshape((SEQS, TOPK))
    route_scores = jnp.clip(jnp.exp(math.log(1.0) - 2.3025851 * jax.random.uniform(seeds[14], (SEQS, TOPK), jnp.float32) ** level_of(seeds[14], (SEQS, TOPK), ((0, 8),), -0.2, 0.2)), 0.1, 1.0)
    w_gate = bell_draw(seeds[15], (EXPERTS, D, FF), D ** -0.5, 0.125, ((0, 8), (2, 4)))
    w_up = bell_draw(seeds[16], (EXPERTS, D, FF), D ** -0.5, 0.125, ((0, 8), (2, 4)))
    w_down = bell_draw(seeds[17], (EXPERTS, FF, D), FF ** -0.5, 0.25, ((0, 8), (1, 4)))
    return dict(tokens=tokens, pre_gain=pre_gain, w_query=w_query, w_forget=w_forget, w_input=w_input, w_outgate=w_outgate, lower_bound=lower_bound, head_gain=head_gain, w_output=w_output, mix_gain=mix_gain, ffn_gain=ffn_gain, post_gain=post_gain, state=state, routes=routes, route_scores=route_scores, w_gate=w_gate, w_up=w_up, w_down=w_down)


EPSILON = 1e-06

def rms_scale(values, gain):
    floats = values.astype(jnp.float32)
    return floats * lax.rsqrt(lax.optimization_barrier(jnp.mean(floats * floats, axis=-1, keepdims=True)) + EPSILON) * gain

def blocked_dot(left, right):
    block_size = left.shape[-1] // N_TP
    running = jnp.zeros((left.shape[0], right.shape[1]), jnp.float32)
    for block_index in range(N_TP):
        lower = block_index * block_size
        partial_value = jnp.dot(left[:, lower:lower + block_size], right[lower:lower + block_size], preferred_element_type=jnp.float32).astype(jnp.bfloat16)
        running = running + lax.optimization_barrier(partial_value).astype(jnp.float32)
    return running

def reference(tokens, pre_gain, w_query, w_forget, w_input, w_outgate, lower_bound, head_gain, w_output, mix_gain, ffn_gain, post_gain, state, routes, route_scores, w_gate, w_up, w_down):
    seq_count = tokens.shape[0]
    head_count = state.shape[1]
    head_size = state.shape[2]
    normed = rms_scale(tokens, pre_gain).astype(jnp.bfloat16)
    query_pre, forget_pre, input_pre, gate_pre = [blocked_dot(normed, weight).astype(jnp.bfloat16) for weight in (w_query, w_forget, w_input, w_outgate)]
    forget = lower_bound + (1.0 - lower_bound) * jax.nn.sigmoid(forget_pre.astype(jnp.float32))
    queries = jax.nn.silu(query_pre.astype(jnp.float32))
    shaped = (seq_count, head_count, head_size)
    new_state = forget.reshape(shaped)[..., None] * state + (1.0 - forget).reshape(shaped)[..., None] * input_pre.astype(jnp.float32).reshape(shaped)[..., None, :]
    readout = jnp.einsum('shk,shkv->shv', queries.reshape(shaped), new_state)
    readout = readout * lax.rsqrt(lax.optimization_barrier(jnp.mean(readout * readout, axis=-1, keepdims=True)) + EPSILON)
    readout = readout * head_gain.reshape(head_count, head_size)
    gated_out = (readout.reshape(seq_count, -1) * jax.nn.silu(gate_pre.astype(jnp.float32))).astype(jnp.bfloat16)
    mixer_out = blocked_dot(gated_out, w_output).astype(jnp.bfloat16)
    residual = (tokens.astype(jnp.float32) + rms_scale(mixer_out, mix_gain)).astype(jnp.bfloat16)
    ffn_in = rms_scale(residual, ffn_gain).astype(jnp.bfloat16)
    route_count = routes.shape[1]
    expert_ids = routes.reshape(-1).astype(jnp.int32)
    source_rows = jnp.repeat(ffn_in, route_count, axis=0)

    def one_route(operands):
        token_row, expert_id = operands
        gate_val = jnp.dot(token_row[None], w_gate[expert_id], preferred_element_type=jnp.float32)
        up_val = jnp.dot(token_row[None], w_up[expert_id], preferred_element_type=jnp.float32)
        hidden = (jax.nn.silu(gate_val) * up_val).astype(jnp.bfloat16)
        return blocked_dot(hidden, w_down[expert_id]).astype(jnp.bfloat16)[0]
    expert_rows = lax.map(one_route, (source_rows, expert_ids))
    weights = route_scores / lax.optimization_barrier(jnp.sum(route_scores, axis=-1, keepdims=True))
    combined = lax.optimization_barrier(jnp.sum(expert_rows.astype(jnp.float32).reshape(seq_count, route_count, -1) * weights[..., None], axis=1))
    layer_out = (residual.astype(jnp.float32) + rms_scale(combined, post_gain)).astype(jnp.bfloat16)
    return (layer_out, new_state)
```

```python
import functools

import jax
import jax.numpy as jnp
from jax import lax
from jax.experimental import pallas as pl
from jax.experimental.pallas import tpu as pltpu
from jax.sharding import PartitionSpec as P

CAP = 12


EPSILON = 1e-06


def rms_scale(values, gain):
    floats = values.astype(jnp.float32)
    return floats * lax.rsqrt(jnp.mean(floats * floats, axis=-1, keepdims=True) + EPSILON) * gain


def plain_device(
    tokens,
    pre_gain,
    w_query,
    w_forget,
    w_input,
    w_outgate,
    lower_bound,
    head_gain,
    w_output,
    mix_gain,
    ffn_gain,
    post_gain,
    state,
    routes,
    route_scores,
    w_gate,
    w_up,
    w_down,
):
    row_count, model_width = tokens.shape
    tp_count = lax.axis_size("tp")
    quarter = model_width // tp_count
    tp_index = lax.axis_index("tp")
    ep_index = lax.axis_index("ep")
    heads_here = state.shape[1]
    head_size = state.shape[2]
    normed = rms_scale(tokens, pre_gain).astype(jnp.bfloat16)
    own_block = lax.dynamic_slice_in_dim(normed, tp_index * quarter, quarter, 1)
    block_rows = lax.all_gather(own_block, "ep", axis=0, tiled=True)
    partial_in = jnp.stack(
        [
            jnp.dot(block_rows, weight, preferred_element_type=jnp.float32)
            for weight in (w_query, w_forget, w_input, w_outgate)
        ],
        axis=1,
    ).astype(jnp.bfloat16)
    by_token = lax.all_to_all(partial_in, "ep", split_axis=0, concat_axis=2, tiled=True)
    summed = lax.psum_scatter(
        by_token.astype(jnp.float32).astype(jnp.bfloat16), "tp", scatter_dimension=2, tiled=True
    )
    query_pre = summed[:, 0]
    forget_pre = summed[:, 1]
    input_pre = summed[:, 2]
    gate_pre = summed[:, 3]
    shaped = (row_count, heads_here, head_size)
    forget = lower_bound + (1.0 - lower_bound) * jax.nn.sigmoid(forget_pre.astype(jnp.float32))
    queries = jax.nn.silu(query_pre.astype(jnp.float32))
    new_state = (
        forget.reshape(shaped)[..., None] * state
        + (1.0 - forget).reshape(shaped)[..., None]
        * input_pre.astype(jnp.float32).reshape(shaped)[..., None, :]
    )
    readout = jnp.einsum("shk,shkv->shv", queries.reshape(shaped), new_state)
    readout = readout * lax.rsqrt(jnp.mean(readout * readout, axis=-1, keepdims=True) + EPSILON)
    readout = readout * head_gain.reshape(heads_here, head_size)
    gated_out = (
        readout.reshape(row_count, quarter) * jax.nn.silu(gate_pre.astype(jnp.float32))
    ).astype(jnp.bfloat16)
    partial_out = jnp.dot(
        lax.all_gather(gated_out, "ep", axis=0, tiled=True),
        w_output,
        preferred_element_type=jnp.float32,
    ).astype(jnp.bfloat16)
    out_token = lax.all_to_all(partial_out, "ep", split_axis=0, concat_axis=1, tiled=True)
    mixer_out = lax.psum(out_token.astype(jnp.float32).astype(jnp.bfloat16), "tp")
    residual = (tokens.astype(jnp.float32) + rms_scale(mixer_out, mix_gain)).astype(jnp.bfloat16)
    ffn_in = rms_scale(residual, ffn_gain).astype(jnp.bfloat16)
    route_count = routes.shape[1]
    exp_dev = w_gate.shape[0]
    capacity = CAP
    weights = route_scores / jnp.sum(route_scores, axis=-1, keepdims=True)
    all_routes, all_weights = (
        lax.all_gather(routes.astype(jnp.float32), "ep", axis=0, tiled=True),
        lax.all_gather(weights, "ep", axis=0, tiled=True),
    )
    all_rows = lax.all_gather(ffn_in, "ep", axis=0, tiled=True)
    seq_total = all_rows.shape[0]
    flat_routes = all_routes.astype(jnp.int32).reshape(-1)
    own_ids = ep_index * exp_dev + jnp.arange(exp_dev, dtype=jnp.int32)
    mine = flat_routes[None, :] == own_ids[:, None]
    rank = jnp.cumsum(mine.astype(jnp.int32), axis=1) - 1
    slot_ids = jnp.arange(capacity, dtype=jnp.int32)
    matched = jnp.logical_and(mine[:, None, :], rank[:, None, :] == slot_ids[None, :, None])
    matched = matched.astype(jnp.float32).reshape(exp_dev, capacity, seq_total, route_count)
    placing = jnp.sum(matched, axis=3).astype(jnp.bfloat16)
    selected = jnp.einsum(
        "ecs,sd->ecd", placing, all_rows, preferred_element_type=jnp.float32
    ).astype(jnp.bfloat16)
    gate_val = jnp.einsum("ecd,edf->ecf", selected, w_gate, preferred_element_type=jnp.float32)
    up_val = jnp.einsum("ecd,edf->ecf", selected, w_up, preferred_element_type=jnp.float32)
    hidden = (jax.nn.silu(gate_val) * up_val).astype(jnp.bfloat16)
    partial_value = jnp.einsum(
        "ecf,efd->ecd", hidden, w_down, preferred_element_type=jnp.float32
    ).astype(jnp.bfloat16)
    reduced = lax.psum_scatter(
        partial_value.astype(jnp.float32).astype(jnp.bfloat16),
        "tp",
        scatter_dimension=2,
        tiled=True,
    )
    every_expert = lax.all_gather(reduced, "ep", axis=0, tiled=True)
    slot_rows = every_expert.reshape(-1, reduced.shape[2])
    own_flat = routes.reshape(-1)
    flat_count = own_flat.shape[0]
    own_pos = ep_index * flat_count + jnp.arange(flat_count, dtype=jnp.int32)
    all_pos = jnp.arange(flat_routes.shape[0], dtype=jnp.int32)
    earlier = jnp.logical_and(
        flat_routes[None, :] == own_flat[:, None], all_pos[None, :] < own_pos[:, None]
    )
    own_rank = jnp.sum(earlier.astype(jnp.int32), axis=1)
    picked = slot_rows[own_flat * capacity + own_rank].astype(jnp.float32)
    picked = picked.reshape(row_count, route_count, -1)
    combined_block = jnp.sum(picked * weights[..., None], axis=1)
    combined = lax.all_gather(combined_block, "tp", axis=1, tiled=True)
    layer_out = (residual.astype(jnp.float32) + rms_scale(combined, post_gain)).astype(jnp.bfloat16)
    return (layer_out, new_state)


MESH = pl.DeviceIdType.MESH
F32 = jnp.float32
BF16 = jnp.bfloat16


def silu(values):
    return values / (1.0 + jnp.exp(-values))


def rsqrt_mean(total, count):
    return lax.rsqrt(total / count + EPSILON)


def layer_kernel(
    ep_n,
    tp_n,
    rows,
    pad,
    tokens_h, pre_gain_h, wq_h, wf_h, wi_h, wo_gate_h, lower_h, head_gain_h, w_out_h,
    mix_gain_h, ffn_gain_h, post_gain_h, state_h, routes_h, scores_h, wg_h, wu_h, wd_h,
    layer_ref, new_state_h,
    tok, pre_gain, w_in, lower, head_gain, w_out, mix_gain, ffn_gain, post_gain, state,
    routes, scores, wg, wu, wd,
    tok_f, norm_send, tok_all, norm_all, dense_all, rows_f, tok_rows, dense_rows,
    part_send, part_recv, fcol, qcol, read_rows, gate_all, gate_rows,
    out_send, out_recv, mix_all, res_all, res_f,
    exp_send, exp_recv, comb_all,
    load_sem, store_sem,
    s_norm, r_norm, s_tok, r_tok, s_dense, r_dense, s_part, r_part, s_gate, r_gate,
    s_out, r_out, s_mix, r_mix, s_exp, r_exp, s_comb, r_comb,
    barrier_unused,
):
    me_ep = lax.axis_index("ep")
    me_tp = lax.axis_index("tp")
    width = tok.shape[1]
    quarter = width // tp_n
    cols = w_out.shape[1]
    per_tp = quarter // cols
    heads, hsize = state.shape[1], state.shape[2]
    all_n = ep_n * tp_n
    me = me_ep * tp_n + me_tp
    group = ep_n * pad // tp_n

    loads = [
        (tokens_h, tok), (pre_gain_h, pre_gain), (routes_h, routes), (scores_h, scores),
        (wq_h, w_in.at[0]), (wf_h, w_in.at[1]), (wi_h, w_in.at[2]), (wo_gate_h, w_in.at[3]),
        (lower_h, lower), (head_gain_h, head_gain), (state_h, state), (w_out_h, w_out),
        (mix_gain_h, mix_gain), (ffn_gain_h, ffn_gain), (wg_h.at[0], wg), (wu_h.at[0], wu),
        (wd_h.at[0], wd), (post_gain_h, post_gain),
    ]
    copies = [pltpu.make_async_copy(a, b, load_sem.at[k]) for k, (a, b) in enumerate(loads)]
    for copy in copies:
        copy.start()

    barrier = pltpu.get_barrier_semaphore()

    def greet(k, carry):
        other = lax.rem(me + k, all_n)
        pl.semaphore_signal(
            barrier, inc=1, device_id={"ep": other // tp_n, "tp": lax.rem(other, tp_n)},
            device_id_type=MESH,
        )
        return carry

    lax.fori_loop(1, all_n, greet, 0)

    tok_f[...] = jnp.zeros_like(tok_f)
    dense_own = jnp.zeros((pad, hsize), F32)
    rows_f[...] = jnp.zeros_like(rows_f)
    for k in range(4):
        copies[k].wait()
    tok_f[0:rows, :] = tok[...].astype(F32)
    toks = tok_f[...]
    scale = rsqrt_mean(jnp.sum(toks * toks, axis=-1, keepdims=True), width)
    normed = (toks * scale * pre_gain[...]).astype(BF16)
    for q in range(tp_n):
        norm_send[q] = normed[:, q * quarter : (q + 1) * quarter]
    norm_all[me_ep] = norm_send[me_tp]
    tok_all[me_ep] = toks.astype(BF16)
    lane = lax.broadcasted_iota(jnp.int32, (rows, hsize), 1)
    score = scores[...]
    weight = score / jnp.sum(score, axis=-1, keepdims=True)
    chosen = routes[...]
    dense = jnp.zeros((rows, hsize), F32)
    for r in range(chosen.shape[1]):
        dense = jnp.where(lane == chosen[:, r : r + 1], weight[:, r : r + 1], dense)
    dense_all[me_ep] = dense_own
    dense_all[me_ep, 0:rows, :] = dense

    pl.semaphore_wait(barrier, all_n - 1)

    def to_ep(source, slot, send, recv, k):
        return pltpu.make_async_remote_copy(
            src_ref=source, dst_ref=slot, send_sem=send.at[k], recv_sem=recv.at[k],
            device_id={"ep": lax.rem(me_ep + k, ep_n), "tp": me_tp}, device_id_type=MESH,
        )

    pending = []
    norm_copies = [
        to_ep(norm_send.at[me_tp], norm_all.at[me_ep], s_norm, r_norm, k) for k in range(1, ep_n)
    ]
    for copy in norm_copies:
        copy.start()
    side = [
        to_ep(ref.at[me_ep], ref.at[me_ep], s, r, k)
        for ref, s, r in ((tok_all, s_tok, r_tok), (dense_all, s_dense, r_dense))
        for k in range(1, ep_n)
    ]
    for copy in side:
        copy.start()
    pending += norm_copies + side

    for k in range(4, 8):
        copies[k].wait()
    for copy in norm_copies:
        copy.wait_recv()
    for i in range(ep_n):
        rows_f[pl.ds(pad * i, pad), :] = norm_all[i].astype(F32)
    x = rows_f[...].astype(BF16)
    for m in range(4):
        part = jnp.dot(x, w_in[m], preferred_element_type=F32)
        for i in range(ep_n):
            part_send[i, :, m * cols : (m + 1) * cols] = part[pad * i : pad * (i + 1)].astype(BF16)
    home = me_ep // per_tp
    slot = lax.rem(me_ep, per_tp) * tp_n + me_tp
    for k in range(ep_n):
        target = lax.rem(me_ep + k, ep_n)
        copy = pltpu.make_async_remote_copy(
            src_ref=part_send.at[target], dst_ref=part_recv.at[slot], send_sem=s_part.at[k],
            recv_sem=r_part.at[slot], device_id={"ep": target, "tp": home}, device_id_type=MESH,
        )
        if k == 0:

            @pl.when(home != me_tp)
            def _():
                copy.start()

            @pl.when(home == me_tp)
            def _():
                part_recv[slot] = part_send[me_ep]

            part_home = copy
        else:
            copy.start()
            pending.append(copy)

    for copy in side:
        copy.wait_recv()
    for i in range(ep_n):
        tok_rows[pl.ds(pad * i, pad), :] = tok_all[i].astype(F32)
        dense_rows[pl.ds(pad * i, pad), :] = dense_all[i]
    for k in range(8, 11):
        copies[k].wait()

    for s in range(per_tp * tp_n):
        source_ep = me_tp * per_tp + s // tp_n
        source_tp = s % tp_n
        local = jnp.logical_and(source_ep == me_ep, me_tp == source_tp)

        @pl.when(jnp.logical_not(local))
        def _():
            pltpu.make_async_remote_copy(
                src_ref=part_recv.at[s], dst_ref=part_recv.at[s], send_sem=s_part.at[0],
                recv_sem=r_part.at[s], device_id={"ep": source_ep, "tp": source_tp},
                device_id_type=MESH,
            ).wait_recv()

    sums = []
    for b in range(per_tp):
        total = part_recv[b * tp_n].astype(F32)
        for t in range(1, tp_n):
            total = total + part_recv[b * tp_n + t].astype(F32)
        sums.append(total.astype(BF16).astype(F32))
    query, forget, value, gate = [
        jnp.concatenate([total[:, m * cols : (m + 1) * cols] for total in sums], axis=1)
        for m in range(4)
    ]
    bound = lower[...]
    forget = bound + (1.0 - bound) / (1.0 + jnp.exp(-forget))
    query = silu(query)
    for h in range(heads):
        fcol[pl.ds(pad * h, pad), :] = forget[:, h * hsize : (h + 1) * hsize]
        qcol[pl.ds(pad * h, pad), :] = query[:, h * hsize : (h + 1) * hsize]
    forget_t = fcol[...].T
    query_t = qcol[...].T
    read_rows[...] = jnp.zeros_like(read_rows)
    for s in range(rows):
        for h in range(heads):
            c = pad * h + s
            f = forget_t[:, c : c + 1]
            new = f * state[s, h] + (1.0 - f) * value[s : s + 1, h * hsize : (h + 1) * hsize]
            state[s, h] = new
            read_rows[c : c + 1, :] = jnp.sum(
                query_t[:, c : c + 1] * new, axis=0, keepdims=True
            )
    readout = read_rows[...]
    readout = readout * rsqrt_mean(jnp.sum(readout * readout, axis=-1, keepdims=True), hsize)
    gated = jnp.concatenate([readout[pad * h : pad * (h + 1)] for h in range(heads)], axis=1)
    gate_all[me_ep] = (gated * head_gain[...] * silu(gate)).astype(BF16)

    gate_copies = [
        to_ep(gate_all.at[me_ep], gate_all.at[me_ep], s_gate, r_gate, k) for k in range(1, ep_n)
    ]
    for copy in gate_copies:
        copy.start()
    pending += gate_copies
    state_out = pltpu.make_async_copy(state, new_state_h, store_sem.at[0])
    state_out.start()

    copies[11].wait()
    for copy in gate_copies:
        copy.wait_recv()
    for i in range(ep_n):
        gate_rows[pl.ds(pad * i, pad), :] = gate_all[i].astype(F32)
    part = jnp.dot(gate_rows[...].astype(BF16), w_out[...], preferred_element_type=F32)
    for t in range(tp_n):
        out_send[t] = part[group * t : group * (t + 1)].astype(BF16)

    def to_tp(source, slot, send, recv, k):
        return pltpu.make_async_remote_copy(
            src_ref=source, dst_ref=slot, send_sem=send.at[k], recv_sem=recv.at[k],
            device_id={"ep": me_ep, "tp": lax.rem(me_tp + k, tp_n)}, device_id_type=MESH,
        )

    out_copies = [
        to_tp(out_send.at[lax.rem(me_tp + k, tp_n)], out_recv.at[me_tp], s_out, r_out, k)
        for k in range(1, tp_n)
    ]
    for copy in out_copies:
        copy.start()
    pending += out_copies
    out_recv[me_tp] = out_send[me_tp]
    for copy in out_copies:
        copy.wait_recv()
    total = out_recv[0].astype(F32)
    for t in range(1, tp_n):
        total = total + out_recv[t].astype(F32)
    mix_all[me] = total.astype(BF16)

    def to_any(source, slot, send, recv, k):
        other = lax.rem(me + k, all_n)
        return pltpu.make_async_remote_copy(
            src_ref=source, dst_ref=slot, send_sem=send.at[k], recv_sem=recv.at[k],
            device_id={"ep": other // tp_n, "tp": lax.rem(other, tp_n)}, device_id_type=MESH,
        )

    def mix_copy(k):
        return to_any(mix_all.at[me], mix_all.at[me], s_mix, r_mix, k)

    lax.fori_loop(1, all_n, lambda k, c: (mix_copy(k).start(), c)[1], 0)
    for k in range(12, 17):
        copies[k].wait()
    lax.fori_loop(1, all_n, lambda k, c: (mix_copy(k).wait_recv(), c)[1], 0)

    mixed = jnp.concatenate(
        [
            jnp.concatenate([mix_all[j * tp_n + t].astype(F32) for t in range(tp_n)], axis=0)
            for j in range(ep_n)
        ],
        axis=1,
    )
    scale = rsqrt_mean(jnp.sum(mixed * mixed, axis=-1, keepdims=True), width)
    residual = (tok_rows[...] + mixed * scale * mix_gain[...]).astype(BF16).astype(F32)
    res_f[...] = residual
    scale = rsqrt_mean(jnp.sum(residual * residual, axis=-1, keepdims=True), width)
    ffn_in = (residual * scale * ffn_gain[...]).astype(BF16)
    for i in range(ep_n):
        res_all[i] = residual[pad * i : pad * (i + 1)]

    gate_val = jnp.dot(ffn_in, wg[...], preferred_element_type=F32)
    up_val = jnp.dot(ffn_in, wu[...], preferred_element_type=F32)
    hidden = (silu(gate_val) * up_val).astype(BF16)
    all_dense = dense_rows[...]
    lane = lax.broadcasted_iota(jnp.int32, all_dense.shape, 1)
    own = jnp.sum(jnp.where(lane == me_ep, all_dense, 0.0), axis=-1, keepdims=True)
    for t in range(tp_n):
        piece = jnp.dot(
            hidden, wd[:, t * quarter : (t + 1) * quarter], preferred_element_type=F32
        )
        piece = jnp.where(own > 0.0, piece * own, 0.0)
        for i in range(ep_n):
            exp_send[i * tp_n + t] = piece[pad * i : pad * (i + 1)].astype(BF16)

    def exp_copy(k):
        return to_any(
            exp_send.at[lax.rem(me + k, all_n)], exp_recv.at[me], s_exp, r_exp, k
        )

    lax.fori_loop(1, all_n, lambda k, c: (exp_copy(k).start(), c)[1], 0)
    exp_recv[me] = exp_send[me]
    lax.fori_loop(1, all_n, lambda k, c: (exp_copy(k).wait_recv(), c)[1], 0)
    total = exp_recv[0].astype(F32)
    for k in range(1, all_n):
        total = total + exp_recv[k].astype(F32)
    comb_all[me_tp] = total
    comb_copies = [
        to_tp(comb_all.at[me_tp], comb_all.at[me_tp], s_comb, r_comb, k) for k in range(1, tp_n)
    ]
    for copy in comb_copies:
        copy.start()
    pending += comb_copies
    copies[17].wait()
    for copy in comb_copies:
        copy.wait_recv()
    combined = jnp.concatenate([comb_all[t] for t in range(tp_n)], axis=1)
    scale = rsqrt_mean(jnp.sum(combined * combined, axis=-1, keepdims=True), width)
    result = (res_all[me_ep] + combined * scale * post_gain[...]).astype(BF16)
    layer_ref[...] = result[0:rows]

    state_out.wait()
    for copy in pending:
        copy.wait_send()

    @pl.when(home != me_tp)
    def _():
        part_home.wait_send()

    lax.fori_loop(1, all_n, lambda k, c: (mix_copy(k).wait_send(), c)[1], 0)
    lax.fori_loop(1, all_n, lambda k, c: (exp_copy(k).wait_send(), c)[1], 0)


def fits(sizes, tokens, w_output, state, w_gate):
    ep_n, tp_n = sizes["ep"], sizes["tp"]
    pad = pl.next_power_of_2(max(tokens.shape[0], 4))
    return (
        w_gate.shape[0] == 1
        and pad <= 8
        and w_output.shape[1] % 128 == 0
        and w_gate.shape[2] % 128 == 0
        and state.shape[2] == 128
        and ep_n <= state.shape[2]
        and ep_n % tp_n == 0
        and (ep_n * pad) % (8 * tp_n) == 0
        and ep_n * tp_n <= 64
    )


def per_device(sizes, *args):
    (
        tokens, pre_gain, w_query, w_forget, w_input, w_outgate, lower_bound, head_gain,
        w_output, mix_gain, ffn_gain, post_gain, state, routes, route_scores, w_gate, w_up,
        w_down,
    ) = args
    if not fits(sizes, tokens, w_output, state, w_gate):
        return plain_device(*args)
    ep_n, tp_n = sizes["ep"], sizes["tp"]
    rows, width = tokens.shape
    pad = pl.next_power_of_2(max(rows, 4))
    quarter = width // tp_n
    cols = w_output.shape[1]
    heads, hsize = state.shape[1], state.shape[2]
    all_n = ep_n * tp_n
    total = ep_n * pad
    group = total // tp_n
    hbm = pl.BlockSpec(memory_space=pl.ANY)
    vmem = pltpu.VMEM
    dma = pltpu.SemaphoreType.DMA
    flat = [
        tokens, pre_gain[None], w_query, w_forget, w_input, w_outgate, lower_bound[None],
        head_gain[None], w_output, mix_gain[None], ffn_gain[None], post_gain[None], state,
        routes, route_scores, w_gate, w_up, w_down,
    ]
    scratch = [
        vmem((rows, width), BF16),
        vmem((1, width), F32),
        vmem((4,) + w_query.shape, BF16),
        vmem((1, quarter), F32),
        vmem((1, quarter), F32),
        vmem(w_output.shape, BF16),
        vmem((1, width), F32),
        vmem((1, width), F32),
        vmem((1, width), F32),
        vmem(state.shape, F32),
        vmem(routes.shape, jnp.int32),
        vmem(route_scores.shape, F32),
        vmem(w_gate.shape[1:], BF16),
        vmem(w_up.shape[1:], BF16),
        vmem(w_down.shape[1:], BF16),
        vmem((pad, width), F32),
        vmem((tp_n, pad, quarter), BF16),
        vmem((ep_n, pad, width), BF16),
        vmem((ep_n, pad, quarter), BF16),
        vmem((ep_n, pad, hsize), F32),
        vmem((total, quarter), F32),
        vmem((total, width), F32),
        vmem((total, hsize), F32),
        vmem((ep_n, pad, 4 * cols), BF16),
        vmem((ep_n, pad, 4 * cols), BF16),
        vmem((heads * pad, hsize), F32),
        vmem((heads * pad, hsize), F32),
        vmem((heads * pad, hsize), F32),
        vmem((ep_n, pad, quarter), BF16),
        vmem((total, quarter), F32),
        vmem((tp_n, group, cols), BF16),
        vmem((tp_n, group, cols), BF16),
        vmem((all_n, group, cols), BF16),
        vmem((ep_n, pad, width), F32),
        vmem((total, width), F32),
        vmem((all_n, pad, quarter), BF16),
        vmem((all_n, pad, quarter), BF16),
        vmem((tp_n, pad, quarter), F32),
        dma((18,)),
        dma((1,)),
    ]
    for count in (ep_n, ep_n, ep_n, ep_n, ep_n, tp_n, all_n, all_n, tp_n):
        scratch += [dma((count,)), dma((count,))]
    scratch.append(pltpu.SemaphoreType.REGULAR)
    return pl.pallas_call(
        functools.partial(layer_kernel, ep_n, tp_n, rows, pad),
        out_shape=(
            jax.ShapeDtypeStruct(tokens.shape, BF16),
            jax.ShapeDtypeStruct(state.shape, F32),
        ),
        in_specs=[hbm] * len(flat),
        out_specs=(pl.BlockSpec(memory_space=pltpu.VMEM), hbm),
        scratch_shapes=scratch,
        compiler_params=pltpu.CompilerParams(collective_id=0, has_side_effects=True),
        name="layer",
    )(*flat)


def solution(mesh):
    in_specs = (
        P("ep", None),
        P(),
        P("tp", "ep"),
        P("tp", "ep"),
        P("tp", "ep"),
        P("tp", "ep"),
        P("tp"),
        P("tp"),
        P("tp", "ep"),
        P(),
        P(),
        P(),
        P("ep", "tp", None, None),
        P("ep", None),
        P("ep", None),
        P("ep", None, "tp"),
        P("ep", None, "tp"),
        P("ep", "tp", None),
    )
    out_specs = (P("ep", None), P("ep", "tp", None, None))
    return jax.shard_map(
        functools.partial(per_device, mesh.shape), mesh=mesh, in_specs=in_specs, out_specs=out_specs, check_vma=False
    )
```

```python
import functools

import jax
import jax.numpy as jnp
from jax import lax
from jax.experimental import pallas as pl
from jax.experimental.pallas import tpu as pltpu
from jax.sharding import PartitionSpec as P

CAP = 12


EPSILON = 1e-06


def rms_scale(values, gain):
    floats = values.astype(jnp.float32)
    return floats * lax.rsqrt(jnp.mean(floats * floats, axis=-1, keepdims=True) + EPSILON) * gain


def plain_device(
    tokens,
    pre_gain,
    w_query,
    w_forget,
    w_input,
    w_outgate,
    lower_bound,
    head_gain,
    w_output,
    mix_gain,
    ffn_gain,
    post_gain,
    state,
    routes,
    route_scores,
    w_gate,
    w_up,
    w_down,
):
    row_count, model_width = tokens.shape
    tp_count = lax.axis_size("tp")
    quarter = model_width // tp_count
    tp_index = lax.axis_index("tp")
    ep_index = lax.axis_index("ep")
    heads_here = state.shape[1]
    head_size = state.shape[2]
    normed = rms_scale(tokens, pre_gain).astype(jnp.bfloat16)
    own_block = lax.dynamic_slice_in_dim(normed, tp_index * quarter, quarter, 1)
    block_rows = lax.all_gather(own_block, "ep", axis=0, tiled=True)
    partial_in = jnp.stack(
        [
            jnp.dot(block_rows, weight, preferred_element_type=jnp.float32)
            for weight in (w_query, w_forget, w_input, w_outgate)
        ],
        axis=1,
    ).astype(jnp.bfloat16)
    by_token = lax.all_to_all(partial_in, "ep", split_axis=0, concat_axis=2, tiled=True)
    summed = lax.psum_scatter(
        by_token.astype(jnp.float32).astype(jnp.bfloat16), "tp", scatter_dimension=2, tiled=True
    )
    query_pre = summed[:, 0]
    forget_pre = summed[:, 1]
    input_pre = summed[:, 2]
    gate_pre = summed[:, 3]
    shaped = (row_count, heads_here, head_size)
    forget = lower_bound + (1.0 - lower_bound) * jax.nn.sigmoid(forget_pre.astype(jnp.float32))
    queries = jax.nn.silu(query_pre.astype(jnp.float32))
    new_state = (
        forget.reshape(shaped)[..., None] * state
        + (1.0 - forget).reshape(shaped)[..., None]
        * input_pre.astype(jnp.float32).reshape(shaped)[..., None, :]
    )
    readout = jnp.einsum("shk,shkv->shv", queries.reshape(shaped), new_state)
    readout = readout * lax.rsqrt(jnp.mean(readout * readout, axis=-1, keepdims=True) + EPSILON)
    readout = readout * head_gain.reshape(heads_here, head_size)
    gated_out = (
        readout.reshape(row_count, quarter) * jax.nn.silu(gate_pre.astype(jnp.float32))
    ).astype(jnp.bfloat16)
    partial_out = jnp.dot(
        lax.all_gather(gated_out, "ep", axis=0, tiled=True),
        w_output,
        preferred_element_type=jnp.float32,
    ).astype(jnp.bfloat16)
    out_token = lax.all_to_all(partial_out, "ep", split_axis=0, concat_axis=1, tiled=True)
    mixer_out = lax.psum(out_token.astype(jnp.float32).astype(jnp.bfloat16), "tp")
    residual = (tokens.astype(jnp.float32) + rms_scale(mixer_out, mix_gain)).astype(jnp.bfloat16)
    ffn_in = rms_scale(residual, ffn_gain).astype(jnp.bfloat16)
    route_count = routes.shape[1]
    exp_dev = w_gate.shape[0]
    capacity = CAP
    weights = route_scores / jnp.sum(route_scores, axis=-1, keepdims=True)
    all_routes, all_weights = (
        lax.all_gather(routes.astype(jnp.float32), "ep", axis=0, tiled=True),
        lax.all_gather(weights, "ep", axis=0, tiled=True),
    )
    all_rows = lax.all_gather(ffn_in, "ep", axis=0, tiled=True)
    seq_total = all_rows.shape[0]
    flat_routes = all_routes.astype(jnp.int32).reshape(-1)
    own_ids = ep_index * exp_dev + jnp.arange(exp_dev, dtype=jnp.int32)
    mine = flat_routes[None, :] == own_ids[:, None]
    rank = jnp.cumsum(mine.astype(jnp.int32), axis=1) - 1
    slot_ids = jnp.arange(capacity, dtype=jnp.int32)
    matched = jnp.logical_and(mine[:, None, :], rank[:, None, :] == slot_ids[None, :, None])
    matched = matched.astype(jnp.float32).reshape(exp_dev, capacity, seq_total, route_count)
    placing = jnp.sum(matched, axis=3).astype(jnp.bfloat16)
    selected = jnp.einsum(
        "ecs,sd->ecd", placing, all_rows, preferred_element_type=jnp.float32
    ).astype(jnp.bfloat16)
    gate_val = jnp.einsum("ecd,edf->ecf", selected, w_gate, preferred_element_type=jnp.float32)
    up_val = jnp.einsum("ecd,edf->ecf", selected, w_up, preferred_element_type=jnp.float32)
    hidden = (jax.nn.silu(gate_val) * up_val).astype(jnp.bfloat16)
    partial_value = jnp.einsum(
        "ecf,efd->ecd", hidden, w_down, preferred_element_type=jnp.float32
    ).astype(jnp.bfloat16)
    reduced = lax.psum_scatter(
        partial_value.astype(jnp.float32).astype(jnp.bfloat16),
        "tp",
        scatter_dimension=2,
        tiled=True,
    )
    every_expert = lax.all_gather(reduced, "ep", axis=0, tiled=True)
    slot_rows = every_expert.reshape(-1, reduced.shape[2])
    own_flat = routes.reshape(-1)
    flat_count = own_flat.shape[0]
    own_pos = ep_index * flat_count + jnp.arange(flat_count, dtype=jnp.int32)
    all_pos = jnp.arange(flat_routes.shape[0], dtype=jnp.int32)
    earlier = jnp.logical_and(
        flat_routes[None, :] == own_flat[:, None], all_pos[None, :] < own_pos[:, None]
    )
    own_rank = jnp.sum(earlier.astype(jnp.int32), axis=1)
    picked = slot_rows[own_flat * capacity + own_rank].astype(jnp.float32)
    picked = picked.reshape(row_count, route_count, -1)
    combined_block = jnp.sum(picked * weights[..., None], axis=1)
    combined = lax.all_gather(combined_block, "tp", axis=1, tiled=True)
    layer_out = (residual.astype(jnp.float32) + rms_scale(combined, post_gain)).astype(jnp.bfloat16)
    return (layer_out, new_state)


MESH = pl.DeviceIdType.MESH
F32 = jnp.float32
BF16 = jnp.bfloat16


def silu(values):
    return values / (1.0 + jnp.exp(-values))


def rsqrt_mean(total, count):
    return lax.rsqrt(total / count + EPSILON)


def layer_kernel(
    ep_n,
    tp_n,
    rows,
    pad,
    tokens_h, pre_gain_h, wq_h, wf_h, wi_h, wo_gate_h, lower_h, head_gain_h, w_out_h,
    mix_gain_h, ffn_gain_h, post_gain_h, state_h, routes_h, scores_h, wg_h, wu_h, wd_h,
    layer_ref, new_state,
    tok, pre_gain, w_in, lower, head_gain, w_out, mix_gain, ffn_gain, post_gain, state,
    routes, scores, wg, wu, wd,
    tok_f, dense_cols, norm_send, tok_all, norm_all, dense_all, rows_f, tok_rows, dense_rows,
    part_send, part_recv, fcol, qcol, read_rows, gate_all, gate_rows,
    out_send, out_recv, mix_all, res_all, res_f,
    exp_send, exp_recv, comb_all,
    load_sem,
    s_norm, r_norm, s_tok, r_tok, s_dense, r_dense, s_part, r_part, s_gate, r_gate,
    s_out, r_out, s_mix, r_mix, s_exp, r_exp, s_comb, r_comb,
):
    me_ep = lax.axis_index("ep")
    me_tp = lax.axis_index("tp")
    width = tok.shape[1]
    quarter = width // tp_n
    cols = w_out.shape[1]
    per_tp = quarter // cols
    heads, hsize = state.shape[1], state.shape[2]
    all_n = ep_n * tp_n
    me = me_ep * tp_n + me_tp
    group = ep_n * pad // tp_n

    loads = [
        (tokens_h, tok), (pre_gain_h, pre_gain), (routes_h, routes), (scores_h, scores),
        (wq_h, w_in.at[0]), (wf_h, w_in.at[1]), (wi_h, w_in.at[2]), (wo_gate_h, w_in.at[3]),
        (lower_h, lower), (head_gain_h, head_gain), (state_h, state), (w_out_h, w_out),
        (mix_gain_h, mix_gain), (ffn_gain_h, ffn_gain), (wg_h.at[0], wg), (wu_h.at[0], wu),
        (wd_h.at[0], wd), (post_gain_h, post_gain),
    ]
    copies = [pltpu.make_async_copy(a, b, load_sem.at[k]) for k, (a, b) in enumerate(loads)]
    for copy in copies:
        copy.start()

    barrier = pltpu.get_barrier_semaphore()

    for k in range(1, ep_n):
        pl.semaphore_signal(
            barrier, inc=1, device_id={"ep": lax.rem(me_ep + k, ep_n), "tp": me_tp},
            device_id_type=MESH,
        )
    for k in range(1, tp_n):
        pl.semaphore_signal(
            barrier, inc=1, device_id={"ep": me_ep, "tp": lax.rem(me_tp + k, tp_n)},
            device_id_type=MESH,
        )

    tok_f[...] = jnp.zeros_like(tok_f)
    dense_cols[...] = jnp.zeros_like(dense_cols)
    rows_f[...] = jnp.zeros_like(rows_f)
    for k in range(2):
        copies[k].wait()
    tok_f[0:rows, :] = tok[...].astype(F32)
    toks = tok_f[...]
    scale = rsqrt_mean(jnp.sum(toks * toks, axis=-1, keepdims=True), width)
    normed = (toks * scale * pre_gain[...]).astype(BF16)
    for q in range(tp_n):
        norm_send[q] = normed[:, q * quarter : (q + 1) * quarter]
    norm_all[me_ep] = norm_send[me_tp]
    tok_all[me_ep] = toks.astype(BF16)
    pl.semaphore_wait(barrier, ep_n + tp_n - 2)

    def to_ep(source, slot, send, recv, k):
        return pltpu.make_async_remote_copy(
            src_ref=source, dst_ref=slot, send_sem=send.at[k], recv_sem=recv.at[k],
            device_id={"ep": lax.rem(me_ep + k, ep_n), "tp": me_tp}, device_id_type=MESH,
        )

    pending = []
    norm_copies = [
        to_ep(norm_send.at[me_tp], norm_all.at[me_ep], s_norm, r_norm, k) for k in range(1, ep_n)
    ]
    for copy in norm_copies:
        copy.start()
    for k in range(2, 4):
        copies[k].wait()
    expert = lax.broadcasted_iota(jnp.int32, (hsize, rows), 0)
    score = scores[...]
    weight = score / jnp.sum(score, axis=0, keepdims=True)
    chosen = routes[...]
    dense = jnp.zeros((hsize, rows), F32)
    for r in range(chosen.shape[0]):
        dense = jnp.where(expert == chosen[r : r + 1, :], weight[r : r + 1, :], dense)
    dense_cols[:, 0:rows] = dense
    dense_all[me_ep] = dense_cols[...].T[0:pad]
    side = [
        to_ep(ref.at[me_ep], ref.at[me_ep], s, r, k)
        for ref, s, r in ((tok_all, s_tok, r_tok), (dense_all, s_dense, r_dense))
        for k in range(1, ep_n)
    ]
    for copy in side:
        copy.start()
    pending += norm_copies + side

    for k in range(4, 8):
        copies[k].wait()
    for copy in norm_copies:
        copy.wait_recv()
    for i in range(ep_n):
        rows_f[pl.ds(pad * i, pad), :] = norm_all[i].astype(F32)
    x = rows_f[...].astype(BF16)
    for m in range(4):
        part = jnp.dot(x, w_in[m], preferred_element_type=F32)
        for i in range(ep_n):
            part_send[i, :, m * cols : (m + 1) * cols] = part[pad * i : pad * (i + 1)].astype(BF16)
    home = me_ep // per_tp
    slot = lax.rem(me_ep, per_tp) * tp_n + me_tp
    for k in range(ep_n):
        target = lax.rem(me_ep + k, ep_n)
        copy = pltpu.make_async_remote_copy(
            src_ref=part_send.at[target], dst_ref=part_recv.at[slot], send_sem=s_part.at[k],
            recv_sem=r_part.at[slot], device_id={"ep": target, "tp": home}, device_id_type=MESH,
        )
        if k == 0:

            @pl.when(home != me_tp)
            def _():
                copy.start()

            @pl.when(home == me_tp)
            def _():
                part_recv[slot] = part_send[me_ep]

            part_home = copy
        else:
            copy.start()
            pending.append(copy)

    for copy in side:
        copy.wait_recv()
    for i in range(ep_n):
        tok_rows[pl.ds(pad * i, pad), :] = tok_all[i].astype(F32)
        dense_rows[pl.ds(pad * i, pad), :] = dense_all[i]
    for k in range(8, 11):
        copies[k].wait()

    for s in range(per_tp * tp_n):
        source_ep = me_tp * per_tp + s // tp_n
        source_tp = s % tp_n
        local = jnp.logical_and(source_ep == me_ep, me_tp == source_tp)

        @pl.when(jnp.logical_not(local))
        def _():
            pltpu.make_async_remote_copy(
                src_ref=part_recv.at[s], dst_ref=part_recv.at[s], send_sem=s_part.at[0],
                recv_sem=r_part.at[s], device_id={"ep": source_ep, "tp": source_tp},
                device_id_type=MESH,
            ).wait_recv()

    sums = []
    for b in range(per_tp):
        total = part_recv[b * tp_n].astype(F32)
        for t in range(1, tp_n):
            total = total + part_recv[b * tp_n + t].astype(F32)
        sums.append(total.astype(BF16).astype(F32))
    query, forget, value, gate = [
        jnp.concatenate([total[:, m * cols : (m + 1) * cols] for total in sums], axis=1)
        for m in range(4)
    ]
    bound = lower[...]
    forget = bound + (1.0 - bound) / (1.0 + jnp.exp(-forget))
    query = silu(query)
    for h in range(heads):
        fcol[pl.ds(pad * h, pad), :] = forget[:, h * hsize : (h + 1) * hsize]
        qcol[pl.ds(pad * h, pad), :] = query[:, h * hsize : (h + 1) * hsize]
    forget_t = fcol[...].T
    query_t = qcol[...].T
    read_rows[...] = jnp.zeros_like(read_rows)
    for s in range(rows):
        for h in range(heads):
            c = pad * h + s
            f = forget_t[:, c : c + 1]
            new = f * state[s, h] + (1.0 - f) * value[s : s + 1, h * hsize : (h + 1) * hsize]
            new_state[s, h] = new
            read_rows[c : c + 1, :] = jnp.sum(
                query_t[:, c : c + 1] * new, axis=0, keepdims=True
            )
    readout = read_rows[...]
    readout = readout * rsqrt_mean(jnp.sum(readout * readout, axis=-1, keepdims=True), hsize)
    gated = jnp.concatenate([readout[pad * h : pad * (h + 1)] for h in range(heads)], axis=1)
    gate_all[me_ep] = (gated * head_gain[...] * silu(gate)).astype(BF16)

    gate_copies = [
        to_ep(gate_all.at[me_ep], gate_all.at[me_ep], s_gate, r_gate, k) for k in range(1, ep_n)
    ]
    for copy in gate_copies:
        copy.start()
    pending += gate_copies

    copies[11].wait()
    for copy in gate_copies:
        copy.wait_recv()
    for i in range(ep_n):
        gate_rows[pl.ds(pad * i, pad), :] = gate_all[i].astype(F32)
    part = jnp.dot(gate_rows[...].astype(BF16), w_out[...], preferred_element_type=F32)
    for t in range(tp_n):
        out_send[t] = part[group * t : group * (t + 1)].astype(BF16)

    def to_tp(source, slot, send, recv, k):
        return pltpu.make_async_remote_copy(
            src_ref=source, dst_ref=slot, send_sem=send.at[k], recv_sem=recv.at[k],
            device_id={"ep": me_ep, "tp": lax.rem(me_tp + k, tp_n)}, device_id_type=MESH,
        )

    out_copies = [
        to_tp(out_send.at[lax.rem(me_tp + k, tp_n)], out_recv.at[me_tp], s_out, r_out, k)
        for k in range(1, tp_n)
    ]
    for copy in out_copies:
        copy.start()
    pending += out_copies
    out_recv[me_tp] = out_send[me_tp]
    for copy in out_copies:
        copy.wait_recv()
    total = out_recv[0].astype(F32)
    for t in range(1, tp_n):
        total = total + out_recv[t].astype(F32)
    mix_all[me] = total.astype(BF16)

    def to_any(source, slot, send, recv, k):
        other = lax.rem(me + k, all_n)
        return pltpu.make_async_remote_copy(
            src_ref=source, dst_ref=slot, send_sem=send.at[k], recv_sem=recv.at[k],
            device_id={"ep": other // tp_n, "tp": lax.rem(other, tp_n)}, device_id_type=MESH,
        )

    def mix_copy(k):
        return to_any(mix_all.at[me], mix_all.at[me], s_mix, r_mix, k)

    lax.fori_loop(1, all_n, lambda k, c: (mix_copy(k).start(), c)[1], 0)
    for k in range(12, 17):
        copies[k].wait()
    lax.fori_loop(1, all_n, lambda k, c: (mix_copy(k).wait_recv(), c)[1], 0)

    mixed = jnp.concatenate(
        [
            jnp.concatenate([mix_all[j * tp_n + t].astype(F32) for t in range(tp_n)], axis=0)
            for j in range(ep_n)
        ],
        axis=1,
    )
    scale = rsqrt_mean(jnp.sum(mixed * mixed, axis=-1, keepdims=True), width)
    residual = (tok_rows[...] + mixed * scale * mix_gain[...]).astype(BF16).astype(F32)
    res_f[...] = residual
    scale = rsqrt_mean(jnp.sum(residual * residual, axis=-1, keepdims=True), width)
    ffn_in = (residual * scale * ffn_gain[...]).astype(BF16)
    for i in range(ep_n):
        res_all[i] = residual[pad * i : pad * (i + 1)]

    gate_val = jnp.dot(ffn_in, wg[...], preferred_element_type=F32)
    up_val = jnp.dot(ffn_in, wu[...], preferred_element_type=F32)
    hidden = (silu(gate_val) * up_val).astype(BF16)
    all_dense = dense_rows[...]
    lane = lax.broadcasted_iota(jnp.int32, all_dense.shape, 1)
    own = jnp.sum(jnp.where(lane == me_ep, all_dense, 0.0), axis=-1, keepdims=True)
    for t in range(tp_n):
        piece = jnp.dot(
            hidden, wd[:, t * quarter : (t + 1) * quarter], preferred_element_type=F32
        )
        piece = jnp.where(own > 0.0, piece * own, 0.0)
        for i in range(ep_n):
            exp_send[i * tp_n + t] = piece[pad * i : pad * (i + 1)].astype(BF16)

    def exp_copy(k):
        return to_any(
            exp_send.at[lax.rem(me + k, all_n)], exp_recv.at[me], s_exp, r_exp, k
        )

    lax.fori_loop(1, all_n, lambda k, c: (exp_copy(k).start(), c)[1], 0)
    exp_recv[me] = exp_send[me]
    lax.fori_loop(1, all_n, lambda k, c: (exp_copy(k).wait_recv(), c)[1], 0)
    total = exp_recv[0].astype(F32)
    for k in range(1, all_n):
        total = total + exp_recv[k].astype(F32)
    comb_all[me_tp] = total
    comb_copies = [
        to_tp(comb_all.at[me_tp], comb_all.at[me_tp], s_comb, r_comb, k) for k in range(1, tp_n)
    ]
    for copy in comb_copies:
        copy.start()
    pending += comb_copies
    copies[17].wait()
    for copy in comb_copies:
        copy.wait_recv()
    combined = jnp.concatenate([comb_all[t] for t in range(tp_n)], axis=1)
    scale = rsqrt_mean(jnp.sum(combined * combined, axis=-1, keepdims=True), width)
    result = (res_all[me_ep] + combined * scale * post_gain[...]).astype(BF16)
    layer_ref[...] = result[0:rows]

    for copy in pending:
        copy.wait_send()

    @pl.when(home != me_tp)
    def _():
        part_home.wait_send()

    lax.fori_loop(1, all_n, lambda k, c: (mix_copy(k).wait_send(), c)[1], 0)
    lax.fori_loop(1, all_n, lambda k, c: (exp_copy(k).wait_send(), c)[1], 0)


def store_kernel(layer, state, layer_h, state_h, sem):
    copies = [
        pltpu.make_async_copy(state, state_h, sem.at[0]),
        pltpu.make_async_copy(layer, layer_h, sem.at[1]),
    ]
    for copy in copies:
        copy.start()
    for copy in copies:
        copy.wait()


def fits(sizes, tokens, w_output, state, w_gate):
    ep_n, tp_n = sizes["ep"], sizes["tp"]
    pad = pl.next_power_of_2(max(tokens.shape[0], 4))
    return (
        w_gate.shape[0] == 1
        and pad <= 8
        and w_output.shape[1] % 128 == 0
        and w_gate.shape[2] % 128 == 0
        and state.shape[2] == 128
        and ep_n <= state.shape[2]
        and ep_n % tp_n == 0
        and (ep_n * pad) % (8 * tp_n) == 0
        and ep_n * tp_n <= 64
    )


def per_device(sizes, *args):
    (
        tokens, pre_gain, w_query, w_forget, w_input, w_outgate, lower_bound, head_gain,
        w_output, mix_gain, ffn_gain, post_gain, state, routes, route_scores, w_gate, w_up,
        w_down,
    ) = args
    if not fits(sizes, tokens, w_output, state, w_gate):
        return plain_device(*args)
    ep_n, tp_n = sizes["ep"], sizes["tp"]
    rows, width = tokens.shape
    pad = pl.next_power_of_2(max(rows, 4))
    quarter = width // tp_n
    cols = w_output.shape[1]
    heads, hsize = state.shape[1], state.shape[2]
    all_n = ep_n * tp_n
    total = ep_n * pad
    group = total // tp_n
    hbm = pl.BlockSpec(memory_space=pltpu.HBM)
    vmem = pltpu.VMEM
    dma = pltpu.SemaphoreType.DMA
    flat = [
        tokens, pre_gain[None], w_query, w_forget, w_input, w_outgate, lower_bound[None],
        head_gain[None], w_output, mix_gain[None], ffn_gain[None], post_gain[None], state,
        routes.T, route_scores.T, w_gate, w_up, w_down,
    ]
    scratch = [
        vmem((rows, width), BF16),
        vmem((1, width), F32),
        vmem((4,) + w_query.shape, BF16),
        vmem((1, quarter), F32),
        vmem((1, quarter), F32),
        vmem(w_output.shape, BF16),
        vmem((1, width), F32),
        vmem((1, width), F32),
        vmem((1, width), F32),
        vmem(state.shape, F32),
        vmem(routes.shape[::-1], jnp.int32),
        vmem(route_scores.shape[::-1], F32),
        vmem(w_gate.shape[1:], BF16),
        vmem(w_up.shape[1:], BF16),
        vmem(w_down.shape[1:], BF16),
        vmem((pad, width), F32),
        vmem((hsize, hsize), F32),
        vmem((tp_n, pad, quarter), BF16),
        vmem((ep_n, pad, width), BF16),
        vmem((ep_n, pad, quarter), BF16),
        vmem((ep_n, pad, hsize), F32),
        vmem((total, quarter), F32),
        vmem((total, width), F32),
        vmem((total, hsize), F32),
        vmem((ep_n, pad, 4 * cols), BF16),
        vmem((ep_n, pad, 4 * cols), BF16),
        vmem((heads * pad, hsize), F32),
        vmem((heads * pad, hsize), F32),
        vmem((heads * pad, hsize), F32),
        vmem((ep_n, pad, quarter), BF16),
        vmem((total, quarter), F32),
        vmem((tp_n, group, cols), BF16),
        vmem((tp_n, group, cols), BF16),
        vmem((all_n, group, cols), BF16),
        vmem((ep_n, pad, width), F32),
        vmem((total, width), F32),
        vmem((all_n, pad, quarter), BF16),
        vmem((all_n, pad, quarter), BF16),
        vmem((tp_n, pad, quarter), F32),
        dma((18,)),
    ]
    for count in (ep_n, ep_n, ep_n, ep_n, ep_n, tp_n, all_n, all_n, tp_n):
        scratch += [dma((count,)), dma((count,))]
    shapes = (
        jax.ShapeDtypeStruct(tokens.shape, BF16),
        jax.ShapeDtypeStruct(state.shape, F32),
    )
    held = pl.pallas_call(
        functools.partial(layer_kernel, ep_n, tp_n, rows, pad),
        out_shape=(pltpu.VMEM(tokens.shape, BF16), pltpu.VMEM(state.shape, F32)),
        in_specs=[hbm] * len(flat),
        out_specs=(pl.BlockSpec(memory_space=pltpu.VMEM),) * 2,
        scratch_shapes=scratch,
        compiler_params=pltpu.CompilerParams(
            collective_id=0, has_side_effects=True, vmem_limit_bytes=60 * 1024 * 1024
        ),
        name="layer",
    )(*flat)
    return pl.pallas_call(
        store_kernel,
        out_shape=shapes,
        in_specs=[pl.BlockSpec(memory_space=pltpu.VMEM)] * 2,
        out_specs=(hbm,) * 2,
        scratch_shapes=[dma((2,))],
        compiler_params=pltpu.CompilerParams(vmem_limit_bytes=4096 * 1024),
        name="store",
    )(*held)


def solution(mesh):
    in_specs = (
        P("ep", None),
        P(),
        P("tp", "ep"),
        P("tp", "ep"),
        P("tp", "ep"),
        P("tp", "ep"),
        P("tp"),
        P("tp"),
        P("tp", "ep"),
        P(),
        P(),
        P(),
        P("ep", "tp", None, None),
        P("ep", None),
        P("ep", None),
        P("ep", None, "tp"),
        P("ep", None, "tp"),
        P("ep", "tp", None),
    )
    out_specs = (P("ep", None), P("ep", "tp", None, None))
    return jax.shard_map(
        functools.partial(per_device, mesh.shape), mesh=mesh, in_specs=in_specs, out_specs=out_specs, check_vma=False
    )
```
